32 devices in a mesh: ep: 8 (over z, y), tp: 4 (over x, core).
Axes of the slice: x: 2, y: 2, z: 4, core: 2. Of those that a mesh axis runs over, the one named last changes fastest.
Arguments:
- query_rows: bfloat16 [4096, 2048], P('ep', 'tp'), may hold values from -6 to 6
- key_rows: bfloat16 [4096, 512], P('ep', 'tp'), may hold values from -6 to 6
- value_rows: bfloat16 [4096, 512], P('ep', 'tp'), may hold values from -6 to 6
- query_gain: float32 [64], replicated, may hold values from 0.2 to 4.5
- key_gain: float32 [64], replicated, may hold values from 0.2 to 4.5
- sink_logit: float32 [32], P('tp'), may hold values from 2 to 6
- out_weight: bfloat16 [2048, 2048], P('tp'), may hold values from -0.125 to 0.125
- tokens: bfloat16 [4096, 2048], P('ep'), may hold values from -6 to 6
- norm_gain: float32 [2048], replicated, may hold values from 0.1 to 1.9
- expert_ids: int32 [4096, 2], P('ep'), may hold values from 0 to 31, all different within a row; in each aligned block of 128 rows (0 to 127, 128 to 255, ...) at most 16 rows name the same one
- route_weight: float32 [4096, 2], P('ep'), may hold values from 0.2 to 1
- gate_weight: bfloat16 [32, 2048, 1024], P('ep', None, 'tp'), may hold values from -0.125 to 0.125
- up_weight: bfloat16 [32, 2048, 1024], P('ep', None, 'tp'), may hold values from -0.125 to 0.125
- down_weight: bfloat16 [32, 1024, 2048], P('ep', 'tp'), may hold values from -0.1875 to 0.1875
- shared_gate: bfloat16 [2048, 1024], P(None, 'tp'), may hold values from -0.125 to 0.125
- shared_up: bfloat16 [2048, 1024], P(None, 'tp'), may hold values from -0.125 to 0.125
- shared_down: bfloat16 [1024, 2048], P('tp'), may hold values from -0.1875 to 0.1875
Outputs:
- mixer_out: bfloat16 [4096, 2048], P(('ep', 'tp'))
- expert_out: bfloat16 [4096, 2048], P(('ep', 'tp'))
The draws below stay inside these ranges and needn't reach their ends.
Inputs may be any that keep to these rules, and one draw needn't show every extreme that they name: `expert_ids`: each row names 2 different experts. In each aligned block of 128 rows no expert is named by more than 16 rows, a bound that some block reaches.
All inputs are finite; a program needn't handle non-finite values.
Results may differ from the reference program's by a relative error of at most 0.012.
The reference program's roundings to bfloat16 on the way count: a program that leaves them out, or rounds other values in their place, can miss the bound.
Values may be sent and summed in bfloat16 or wider, within the bound.
A program may use at most 128 MiB of HBM per device.

```python
import math
import jax
import jax.numpy as jnp
import numpy as np
from jax import lax

D = 2048
HEADS = 32
KV_HEADS = 8
HEAD_DIM = 64
FF = 1024
WINDOW = 128
BLOCK = 128
TOP_K = 2
B_ROWS = 128
EXPERTS = 32
CAP = 16
TOKENS_A = 4096
TOKENS_B = 4096
N_TP = 4


def attention_pair(key):
    base = jax.random.fold_in(key, 7001)
    first_key, second_key = jax.random.split(base)
    key_values = jax.random.normal(first_key, (TOKENS_A, KV_HEADS * HEAD_DIM), jnp.float32)
    query_values = jax.random.normal(second_key, (TOKENS_A, HEADS * HEAD_DIM), jnp.float32)
    return (jnp.clip(query_values, -6.0, 6.0), jnp.clip(key_values, -6.0, 6.0))


def gain_draw(key):
    return jnp.clip(1.0 + 0.18 * jax.random.normal(key, (HEAD_DIM,), jnp.float32), 0.2, 1.8)


def draw_query_rows(key, part):
    return attention_pair(key)[0].astype(jnp.bfloat16)


def draw_key_rows(key, part):
    return attention_pair(key)[1].astype(jnp.bfloat16)


def draw_query_gain(key, part):
    return gain_draw(jax.random.fold_in(key, 31))


def draw_key_gain(key, part):
    return gain_draw(jax.random.fold_in(key, 47))


def steps_of(stream_key, dims, cuts, low, high):
    factor_of = 1.0
    for axis_at, shards_of in cuts:
        steps = jax.random.uniform(jax.random.fold_in(jax.random.fold_in(stream_key, 6), axis_at), (shards_of,), jnp.float32, low / len(cuts), high / len(cuts))
        factor_of = factor_of * jnp.repeat(jnp.exp(steps), dims[axis_at] // shards_of).reshape((-1,) + (1,) * (len(dims) - 1 - axis_at))
    return factor_of


def assign_block(rng, own, number, rows, amount, top, limit, skew):
    order = jax.random.permutation(rng, amount)
    heavy_load, usual = load_shares(amount, rows * top, limit, skew, True), load_shares(amount, rows * top, limit, skew, False)
    places = jnp.arange(amount)

    def named(tallies, turn):
        used = int((tallies > 0).sum())
        fixed = max(1, used // 4)
        moved = fixed + (places - fixed + turn * (used - fixed)) % max(1, amount - fixed)
        return jnp.zeros((amount,), jnp.int32).at[order[jnp.where(places < fixed, places, moved)]].set(jnp.asarray(tallies, jnp.int32))

    tallies = jnp.where(number % 4 == 0, named(heavy_load, number // 4), named(usual, number - number // 4 - 1))
    mixed = jax.random.permutation(jax.random.fold_in(own, 3), amount)
    giver, taker = mixed[0:amount // 2 * 2:2], mixed[1:amount // 2 * 2:2]
    room = jnp.minimum(tallies[giver] - 1, limit - tallies[taker]) // 2
    room = jnp.where((giver == order[0]) | (taker == order[0]) | (tallies[taker] == 0), 0, jnp.maximum(room, 0))
    moved = jax.random.randint(jax.random.fold_in(own, 4), (amount // 2,), 0, 1 << 20) % (room + 1)
    tallies = tallies.at[giver].add(-moved).at[taker].add(moved)
    labels = jnp.searchsorted(jnp.cumsum(tallies), jnp.arange(rows * top), side="right").astype(jnp.int32)
    listing = labels.reshape(top, rows).T
    listing = listing[jax.random.permutation(jax.random.fold_in(own, 1), rows)]
    turn = jax.random.randint(jax.random.fold_in(own, 2), (rows, 1), 0, top)
    return jnp.take_along_axis(listing, (jnp.arange(top)[None, :] + turn) % top, axis=1)


def load_shares(count, total, limit, lean, full):
    weights = [(1 << 20) // math.isqrt(grade ** lean) + 1 for grade in range(1, count + 1)]
    largest = limit if full else min(limit, max(-(-total // count), total * weights[0] // sum(weights)))
    least = 1 if total - largest >= count - 1 else 0
    given, surplus = [largest] + [least] * (count - 1), total - largest - least * (count - 1)
    while surplus > 0:
        candidates = [i for i in range(1, count) if given[i] < largest] or [i for i in range(1, count) if given[i] < limit]
        pool, remaining = sum([weights[i] for i in candidates]), surplus
        for i in candidates:
            addition = min(limit - given[i], max(1, remaining * weights[i] // pool), surplus)
            given[i] = given[i] + addition
            surplus = surplus - addition
    return np.array(given)


def scatter_about(own_key, extent, width, bound, pieces=(), kind=jnp.bfloat16):
    result = width * jax.random.normal(own_key, extent, jnp.float32)
    if pieces:
        result = result * steps_of(own_key, extent, pieces, -0.22, 0.18)
    return jnp.clip(result, -bound, bound).astype(kind)


def setup_inputs(seed: int = 0) -> dict:
    key_list = jax.random.split(jax.random.key(seed), 18)
    query_rows = draw_query_rows(jax.random.fold_in(key_list[17], 71), 0)
    key_rows = draw_key_rows(jax.random.fold_in(key_list[17], 71), 0)
    value_rows = scatter_about(key_list[2], (TOKENS_A, KV_HEADS * HEAD_DIM), 1.0, 6.0, ((0, 8), (1, 4)))
    query_gain = draw_query_gain(jax.random.fold_in(key_list[17], 71), 0)
    key_gain = draw_key_gain(jax.random.fold_in(key_list[17], 71), 0)
    sink_logit = jnp.clip(2.0 + 4.0 * jax.random.uniform(key_list[5], (HEADS,), jnp.float32) ** steps_of(key_list[5], (HEADS,), ((0, 4),), -0.2, 0.2), 2.0, 6.0)
    out_weight = scatter_about(key_list[6], (HEADS * HEAD_DIM, D), (HEADS * HEAD_DIM) ** -0.5, 0.125, ((0, 4),))
    tokens = scatter_about(key_list[7], (TOKENS_B, D), 1.0, 6.0, ((0, 8),))
    norm_gain = jnp.clip(1.0 + 0.18 * jax.random.normal(key_list[8], (D,), jnp.float32), 0.1, 1.9)
    expert_ids_keys = jax.random.split(jax.random.fold_in(key_list[9], 1), TOKENS_B // B_ROWS)
    expert_ids_turns = jax.random.permutation(jax.random.fold_in(key_list[9], 3), TOKENS_B // B_ROWS)
    expert_ids = jax.vmap(lambda own, number: assign_block(jax.random.fold_in(key_list[9], 2), own, number, B_ROWS, EXPERTS, TOP_K, CAP, 1))(expert_ids_keys, expert_ids_turns).reshape((TOKENS_B, TOP_K))
    route_weight = jnp.clip(0.2 + 0.8 * jax.random.uniform(key_list[10], (TOKENS_B, TOP_K), jnp.float32) ** steps_of(key_list[10], (TOKENS_B, TOP_K), ((0, 8),), -0.2, 0.2), 0.2, 1.0)
    gate_weight = scatter_about(key_list[11], (EXPERTS, D, FF), D ** -0.5, 0.125, ((0, 8), (2, 4)))
    up_weight = scatter_about(key_list[12], (EXPERTS, D, FF), D ** -0.5, 0.125, ((0, 8), (2, 4)))
    down_weight = scatter_about(key_list[13], (EXPERTS, FF, D), FF ** -0.5, 0.1875, ((0, 8), (1, 4)))
    shared_gate = scatter_about(key_list[14], (D, FF), D ** -0.5, 0.125, ((1, 4),))
    shared_up = scatter_about(key_list[15], (D, FF), D ** -0.5, 0.125, ((1, 4),))
    shared_down = scatter_about(key_list[16], (FF, D), FF ** -0.5, 0.1875, ((0, 4),))
    return {"query_rows": query_rows, "key_rows": key_rows, "value_rows": value_rows, "query_gain": query_gain, "key_gain": key_gain, "sink_logit": sink_logit, "out_weight": out_weight, "tokens": tokens, "norm_gain": norm_gain, "expert_ids": expert_ids, "route_weight": route_weight, "gate_weight": gate_weight, "up_weight": up_weight, "down_weight": down_weight, "shared_gate": shared_gate, "shared_up": shared_up, "shared_down": shared_down}


epsilon = 1e-06
masked_score = -1e+30

def rms_scale(values, gain):
    widened = values.astype(jnp.float32)
    scaled = widened * lax.rsqrt(lax.optimization_barrier(jnp.mean(widened * widened, axis=-1, keepdims=True)) + epsilon)
    return (scaled * gain).astype(jnp.bfloat16)

def rounded_sum(hidden, weight):
    group_width = hidden.shape[-1] // N_TP
    running = jnp.zeros((hidden.shape[0], weight.shape[-1]), jnp.float32)
    for group_index in range(N_TP):
        lower = group_index * group_width
        partial_value = jnp.dot(hidden[:, lower:lower + group_width], weight[lower:lower + group_width], preferred_element_type=jnp.float32)
        running = running + lax.optimization_barrier(partial_value.astype(jnp.bfloat16)).astype(jnp.float32)
    return running.astype(jnp.bfloat16)

def expert_ffn(rows_in, gate_matrix, up_matrix, down_matrix):
    gate_part = jnp.dot(rows_in, gate_matrix, preferred_element_type=jnp.float32)
    up_part = jnp.dot(rows_in, up_matrix, preferred_element_type=jnp.float32)
    hidden = (jax.nn.silu(gate_part) * up_part).astype(jnp.bfloat16)
    return rounded_sum(hidden, down_matrix)

def window_mask(first_block, block_count):
    query_pos = jnp.arange(BLOCK)[:, None]
    key_pos = jnp.arange(2 * BLOCK)[None, :]
    inside = (key_pos <= query_pos + BLOCK) & (key_pos > query_pos + BLOCK - WINDOW)
    not_first = (first_block + jnp.arange(block_count))[:, None, None] > 0
    return inside[None] & (not_first | (key_pos[None] >= BLOCK))

def band_blocks(blocks_in):
    earlier = jnp.concatenate([jnp.zeros_like(blocks_in[:1]), blocks_in[:-1]], axis=0)
    return jnp.concatenate([earlier, blocks_in], axis=1)

def reference(query_rows, key_rows, value_rows, query_gain, key_gain, sink_logit, out_weight, tokens, norm_gain, expert_ids, route_weight, gate_weight, up_weight, down_weight, shared_gate, shared_up, shared_down):
    sequence_rows = query_rows.shape[0]
    blocks = sequence_rows // BLOCK
    group_size = HEADS // KV_HEADS
    query_normed = rms_scale(query_rows.reshape(blocks, BLOCK, KV_HEADS, group_size, HEAD_DIM), query_gain)
    key_normed = rms_scale(key_rows.reshape(blocks, BLOCK, KV_HEADS, HEAD_DIM), key_gain)
    key_band = band_blocks(key_normed)
    value_band = band_blocks(value_rows.reshape(blocks, BLOCK, KV_HEADS, HEAD_DIM))
    window = window_mask(0, blocks)
    score_scale = 1.0 / math.sqrt(HEAD_DIM)

    def one_head(inputs):
        query_head, key_head, value_head, sink_head = inputs
        scores = jnp.einsum('nqgd,nkd->gnqk', query_head.astype(jnp.float32), key_head.astype(jnp.float32)) * score_scale
        scores = jnp.where(window[None], scores, masked_score)
        sink_col = sink_head[:, None, None, None]
        row_max = jnp.maximum(lax.optimization_barrier(jnp.max(scores, axis=-1, keepdims=True)), sink_col)
        exp_scores = jnp.exp(scores - row_max)
        attn_probs = (exp_scores / (lax.optimization_barrier(jnp.sum(exp_scores, axis=-1, keepdims=True)) + jnp.exp(sink_col - row_max))).astype(jnp.bfloat16)
        return jnp.einsum('gnqk,nkd->nqgd', attn_probs.astype(jnp.float32), value_head.astype(jnp.float32)).astype(jnp.bfloat16)
    per_head = lax.map(one_head, (jnp.moveaxis(query_normed, 2, 0), jnp.moveaxis(key_band, 2, 0), jnp.moveaxis(value_band, 2, 0), sink_logit.reshape(KV_HEADS, group_size)))
    heads_out = jnp.moveaxis(per_head, 0, 2).reshape(sequence_rows, HEADS * HEAD_DIM)
    mixer_out = rounded_sum(heads_out, out_weight)
    normed = rms_scale(tokens, norm_gain)
    token_count = tokens.shape[0]
    flat_ids = expert_ids.reshape(-1).astype(jnp.int32)
    assign_count = flat_ids.shape[0]
    span_rows = 128
    sort_order = jnp.argsort(flat_ids, stable=True).astype(jnp.int32)
    sorted_ids = flat_ids[sort_order]
    counts = jnp.zeros((EXPERTS,), jnp.int32).at[flat_ids].add(1)
    starts = (jnp.cumsum(counts) - counts).astype(jnp.int32)
    padded = (counts + span_rows - 1) // span_rows * span_rows
    pad_ends = jnp.cumsum(padded).astype(jnp.int32)
    pad_starts = pad_ends - padded
    target = pad_starts[sorted_ids] + jnp.arange(assign_count, dtype=jnp.int32) - starts[sorted_ids]
    span_count = (assign_count + EXPERTS * (span_rows - 1) + span_rows - 1) // span_rows
    slot_assign = jnp.full((span_count * span_rows,), assign_count, jnp.int32).at[target].set(sort_order)
    span_expert = jnp.minimum(jnp.searchsorted(pad_ends, jnp.arange(span_count, dtype=jnp.int32) * span_rows, side='right'), EXPERTS - 1).astype(jnp.int32)
    padded_rows = jnp.concatenate([normed, jnp.zeros((1, D), jnp.bfloat16)], axis=0)

    def one_span(inputs):
        assigns, expert = inputs
        span_tokens = padded_rows[assigns // TOP_K]
        return expert_ffn(span_tokens, gate_weight[expert], up_weight[expert], down_weight[expert])
    span_out = lax.map(one_span, (slot_assign.reshape(span_count, span_rows), span_expert))
    per_assign = jnp.zeros((assign_count + 1, D), jnp.bfloat16).at[slot_assign].set(span_out.reshape(-1, D))
    routed = per_assign[:assign_count].reshape(token_count, TOP_K, D).astype(jnp.float32)
    shared_out = expert_ffn(normed, shared_gate, shared_up, shared_down)
    expert_out = (shared_out.astype(jnp.float32) + lax.optimization_barrier(jnp.sum(routed * route_weight[:, :, None], axis=1))).astype(jnp.bfloat16)
    return (mixer_out, expert_out)
```

```python
import functools
import jax
import jax.numpy as jnp
from jax import lax
from jax.experimental import pallas as pl
from jax.experimental.pallas import tpu as pltpu
from jax.sharding import PartitionSpec as P

HEADS = 32
KV_HEADS = 8
HEAD_DIM = 64
WINDOW = 128
BLOCK = 128
TOP_K = 2


epsilon = 1e-06
masked_score = -1e30
score_scale = 0.125


def from_behind(block, axis, distance):
    devices = range(lax.axis_size(axis))
    route = [(i - distance, i) for i in devices if i - distance in devices]
    return lax.ppermute(block, axis, route)


def rms_scale(values, gain):
    widened = values.astype(jnp.float32)
    scaled = widened * lax.rsqrt(jnp.mean(widened * widened, axis=-1, keepdims=True) + epsilon)
    return (scaled * gain).astype(jnp.bfloat16)


def window_mask(first_block, block_count):
    query_pos = jnp.arange(BLOCK)[:, None]
    key_pos = jnp.arange(2 * BLOCK)[None, :]
    inside = (key_pos <= query_pos + BLOCK) & (key_pos > query_pos + BLOCK - WINDOW)
    not_first = (first_block + jnp.arange(block_count))[:, None, None] > 0
    return inside[None] & (not_first | (key_pos[None] >= BLOCK))


def band_blocks(rim_block, blocks_in):
    joined = jnp.concatenate([rim_block[None], blocks_in], axis=0)
    return jnp.concatenate([joined[:-1], joined[1:]], axis=1)


def attention_part(query_rows, key_rows, value_rows, query_gain, key_gain, sink_logit):
    sequence_rows = query_rows.shape[0]
    blocks = sequence_rows // BLOCK
    pair_heads = key_rows.shape[1] // HEAD_DIM
    group_size = HEADS // KV_HEADS
    query_normed = rms_scale(
        query_rows.reshape(blocks, BLOCK, pair_heads, group_size, HEAD_DIM), query_gain
    )
    key_normed = rms_scale(key_rows.reshape(blocks, BLOCK, pair_heads, HEAD_DIM), key_gain)
    value_blocks = value_rows.reshape(blocks, BLOCK, pair_heads, HEAD_DIM)
    rim_keys, rim_values = from_behind((key_normed[blocks - 1], value_blocks[blocks - 1]), "ep", 1)
    key_band = band_blocks(rim_keys, key_normed)
    value_band = band_blocks(rim_values, value_blocks)
    window = window_mask(lax.axis_index("ep") * blocks, blocks)
    scores = (
        jnp.einsum("nqhgd,nkhd->hgnqk", query_normed, key_band, preferred_element_type=jnp.float32)
        * score_scale
    )
    scores = jnp.where(window[None, None], scores, masked_score)
    sink_col = sink_logit.reshape(pair_heads, group_size, 1, 1, 1)
    row_max = jnp.maximum(jnp.max(scores, axis=-1, keepdims=True), sink_col)
    exp_scores = jnp.exp(scores - row_max)
    attn_probs = (
        exp_scores / (jnp.sum(exp_scores, axis=-1, keepdims=True) + jnp.exp(sink_col - row_max))
    ).astype(jnp.bfloat16)
    heads_out = (
        jnp.einsum("hgnqk,nkhd->nqhgd", attn_probs, value_band, preferred_element_type=jnp.float32)
        .astype(jnp.bfloat16)
        .reshape(sequence_rows, pair_heads * group_size * HEAD_DIM)
    )
    return heads_out


def exchange_kernel(
    ranks,
    group,
    local_experts,
    capacity,
    outgoing,
    mixer_part,
    shared_part,
    gate,
    up,
    down,
    returned,
    mixer_sum,
    shared_sum,
    rows,
    kept,
    sibling_send,
    sibling_recv,
    peer_send,
    peer_recv,
    finished,
    early_recv,
    early_send,
    early_peer,
    out_sems,
    in_sems,
    fan_send,
    fan_recv,
    add_send,
    add_recv,
    back_send,
    back_recv,
    early_s,
    early_r,
    own_sem,
):
    rank = lax.axis_index("ep")
    part = lax.axis_index("tp")
    sibling = part + 1 - 2 * lax.rem(part, 2)
    peer = lax.rem(part + 2, 4)
    across = 3 - part
    f32, bf16 = jnp.float32, jnp.bfloat16
    mesh_ids = pl.DeviceIdType.MESH

    def send(source, target, send_sem, recv_sem, ep_to, tp_to):
        copy = pltpu.make_async_remote_copy(
            src_ref=source,
            dst_ref=target,
            send_sem=send_sem,
            recv_sem=recv_sem,
            device_id=(ep_to, tp_to),
            device_id_type=mesh_ids,
        )
        copy.start()
        return copy

    barrier = pltpu.get_barrier_semaphore()
    for k in range(1, ranks):
        pl.semaphore_signal(
            barrier, inc=1, device_id=(lax.rem(rank + k, ranks), part), device_id_type=mesh_ids
        )
    for other in (sibling, peer):
        pl.semaphore_signal(barrier, inc=1, device_id=(rank, other), device_id_type=mesh_ids)
    pl.semaphore_wait(barrier, ranks + 1)

    own = pltpu.make_async_copy(outgoing.at[0], rows.at[0, 0], own_sem)
    own.start()
    dispatched = [None] + [
        send(
            outgoing.at[k],
            rows.at[k, 0],
            out_sems.at[k],
            in_sems.at[k],
            lax.rem(rank + k, ranks),
            part,
        )
        for k in range(1, ranks)
    ]
    early = []
    for i, full in enumerate((mixer_part, shared_part)):
        for j, which in enumerate((across, sibling)):
            s = 2 * i + j
            early.append(
                send(
                    full.at[which],
                    early_recv.at[s],
                    early_s.at[s],
                    early_r.at[s],
                    rank,
                    sibling,
                )
            )
    to_sibling = {}
    to_peer = {}
    relayed = {}
    added = {}
    peered = {}
    backs = {}

    def fan_out(k):
        if k == 0:
            own.wait()
        else:
            dispatched[k].wait_recv()
        to_peer[k] = send(
            rows.at[k, 0], rows.at[k, 2], fan_send.at[0, k], fan_recv.at[0, k], rank, peer
        )
        to_sibling[k] = send(
            rows.at[k, 0], rows.at[k, 1], fan_send.at[1, k], fan_recv.at[1, k], rank, sibling
        )

    def relay(k):
        to_peer[k].wait_recv()
        relayed[k] = send(
            rows.at[k, 2], rows.at[k, 3], fan_send.at[2, k], fan_recv.at[2, k], rank, sibling
        )

    def early_add():
        for i, full in enumerate((mixer_part, shared_part)):
            early[2 * i].wait_recv()
            early_send[i] = (
                full[peer].astype(f32) + early_recv[2 * i].astype(f32)
            ).astype(bf16)
            early.append(
                send(
                    early_send.at[i],
                    early_peer.at[i],
                    early_s.at[4 + i],
                    early_r.at[4 + i],
                    rank,
                    peer,
                )
            )

    def early_finish():
        for i, (full, total) in enumerate(((mixer_part, mixer_sum), (shared_part, shared_sum))):
            early[2 * i + 1].wait_recv()
            early[4 + i].wait_recv()
            total[...] = (
                full[part].astype(f32)
                + early_recv[2 * i + 1].astype(f32)
                + early_peer[i].astype(f32)
            ).astype(bf16)

    def experts(g):
        first = g * group
        for k in range(first, first + group):
            to_sibling[k].wait_recv()
            relayed[k].wait_recv()
        width = rows.shape[-1]

        def one(index, carry):
            at = pl.ds(pl.multiple_of(index * capacity, capacity), capacity)
            block = rows[first : first + group, :, at, :].reshape(group * 4 * capacity, width)
            gate_part = jnp.dot(block, gate[index], preferred_element_type=f32)
            up_part = jnp.dot(block, up[index], preferred_element_type=f32)
            hidden = (gate_part / (1.0 + jnp.exp(-gate_part)) * up_part).astype(bf16)
            made = jnp.dot(hidden, down[index], preferred_element_type=f32)
            made = made.astype(bf16).reshape(group, 4, capacity, width)
            spot = pl.ds(first, group)
            kept[spot, 0, at, :] = made[:, 0]
            sibling_send[spot, 0, at, :] = made[:, 1]
            kept[spot, 1, at, :] = made[:, 2]
            sibling_send[spot, 1, at, :] = made[:, 3]
            return carry

        lax.fori_loop(0, local_experts, one, 0)
        for k in range(first, first + group):
            added[k] = send(
                sibling_send.at[k],
                sibling_recv.at[k],
                add_send.at[0, k],
                add_recv.at[0, k],
                rank,
                sibling,
            )

    def pair_add(k):
        added[k].wait_recv()
        peer_send[k] = (kept[k, 1].astype(f32) + sibling_recv[k, 1].astype(f32)).astype(bf16)
        peered[k] = send(
            peer_send.at[k], peer_recv.at[k], add_send.at[1, k], add_recv.at[1, k], rank, peer
        )

    def finish(k):
        peered[k].wait_recv()
        total = (
            kept[k, 0].astype(f32) + sibling_recv[k, 0].astype(f32) + peer_recv[k].astype(f32)
        ).astype(bf16)
        if k == 0:
            returned[0] = total
        else:
            finished[k] = total
            backs[k] = send(
                finished.at[k],
                returned.at[k],
                back_send.at[k],
                back_recv.at[k],
                lax.rem(rank + ranks - k, ranks),
                part,
            )

    groups = ranks // group
    for step in range(groups + 4):
        for stage, work in ((0, fan_out), (1, relay)):
            g = step - stage
            if 0 <= g < groups:
                for k in range(g * group, (g + 1) * group):
                    work(k)
        if step == 0:
            early_add()
        if 0 <= step - 3 < groups:
            for k in range((step - 3) * group, (step - 2) * group):
                pair_add(k)
        if 0 <= step - 2 < groups:
            experts(step - 2)
        if 0 <= step - 4 < groups:
            for k in range((step - 4) * group, (step - 3) * group):
                finish(k)
        if step == 2:
            early_finish()
    for k in range(1, ranks):
        backs[k].wait_recv()
    for k in range(1, ranks):
        dispatched[k].wait_send()
        backs[k].wait_send()
    for table in (to_peer, to_sibling, relayed, added, peered):
        for k in range(ranks):
            table[k].wait_send()
    for copy in early:
        copy.wait_send()


def exchange(outgoing, mixer_part, shared_part, gate, up, down, capacity):
    ranks, share, width = outgoing.shape
    quarter = mixer_part.shape[1]
    local_experts = gate.shape[0]
    group = 2
    bf16 = jnp.bfloat16
    dma = pltpu.SemaphoreType.DMA
    vmem = pl.BlockSpec(memory_space=pltpu.VMEM)
    return pl.pallas_call(
        functools.partial(exchange_kernel, ranks, group, local_experts, capacity),
        out_shape=(
            jax.ShapeDtypeStruct((ranks, share, width), bf16),
            jax.ShapeDtypeStruct((quarter, width), bf16),
            jax.ShapeDtypeStruct((quarter, width), bf16),
        ),
        in_specs=[vmem] * 6,
        out_specs=(vmem,) * 3,
        scratch_shapes=[
            pltpu.VMEM((ranks, 4, share, width), bf16),
            pltpu.VMEM((ranks, 2, share, width), bf16),
            pltpu.VMEM((ranks, 2, share, width), bf16),
            pltpu.VMEM((ranks, 2, share, width), bf16),
            pltpu.VMEM((ranks, share, width), bf16),
            pltpu.VMEM((ranks, share, width), bf16),
            pltpu.VMEM((ranks, share, width), bf16),
            pltpu.VMEM((4, quarter, width), bf16),
            pltpu.VMEM((2, quarter, width), bf16),
            pltpu.VMEM((2, quarter, width), bf16),
            dma((ranks,)),
            dma((ranks,)),
            dma((3, ranks)),
            dma((3, ranks)),
            dma((2, ranks)),
            dma((2, ranks)),
            dma((ranks,)),
            dma((ranks,)),
            dma((6,)),
            dma((6,)),
            dma,
        ],
        compiler_params=pltpu.CompilerParams(
            collective_id=0, has_side_effects=True, vmem_limit_bytes=64000 * 1024
        ),
    )(outgoing, mixer_part, shared_part, gate, up, down)


def wide_shards(
    query_rows,
    key_rows,
    value_rows,
    query_gain,
    key_gain,
    sink_logit,
    out_weight,
    tokens,
    norm_gain,
    expert_ids,
    route_weight,
    gate_weight,
    up_weight,
    down_weight,
    shared_gate,
    shared_up,
    shared_down,
):
    expert_ranks = lax.axis_size("ep")
    head_ranks = lax.axis_size("tp")
    head_rank = lax.axis_index("tp")
    sequence_rows = query_rows.shape[0]
    blocks = sequence_rows // BLOCK
    pair_heads = key_rows.shape[1] // HEAD_DIM
    group_size = HEADS // KV_HEADS
    query_normed = rms_scale(
        query_rows.reshape(blocks, BLOCK, pair_heads, group_size, HEAD_DIM), query_gain
    )
    key_normed = rms_scale(key_rows.reshape(blocks, BLOCK, pair_heads, HEAD_DIM), key_gain)
    value_blocks = value_rows.reshape(blocks, BLOCK, pair_heads, HEAD_DIM)
    rim_keys, rim_values = from_behind((key_normed[blocks - 1], value_blocks[blocks - 1]), "ep", 1)
    key_band = band_blocks(rim_keys, key_normed)
    value_band = band_blocks(rim_values, value_blocks)
    window = window_mask(lax.axis_index("ep") * blocks, blocks)
    scores = (
        jnp.einsum("nqhgd,nkhd->hgnqk", query_normed, key_band, preferred_element_type=jnp.float32)
        * score_scale
    )
    scores = jnp.where(window[None, None], scores, masked_score)
    sink_col = sink_logit.reshape(pair_heads, group_size, 1, 1, 1)
    row_max = jnp.maximum(jnp.max(scores, axis=-1, keepdims=True), sink_col)
    exp_scores = jnp.exp(scores - row_max)
    attn_probs = (
        exp_scores / (jnp.sum(exp_scores, axis=-1, keepdims=True) + jnp.exp(sink_col - row_max))
    ).astype(jnp.bfloat16)
    heads_out = (
        jnp.einsum("hgnqk,nkhd->nqhgd", attn_probs, value_band, preferred_element_type=jnp.float32)
        .astype(jnp.bfloat16)
        .reshape(sequence_rows, pair_heads * group_size * HEAD_DIM)
    )
    local_experts = gate_weight.shape[0]
    expert_total = local_experts * expert_ranks
    quarter = tokens.shape[0] // head_ranks
    model_width = tokens.shape[1]
    capacity = 2 * quarter * TOP_K // expert_total
    slot_share = local_experts * capacity
    routed_rows = expert_ranks * slot_share
    normed = rms_scale(tokens, norm_gain)
    route_ids = expert_ids.reshape(head_ranks, quarter * TOP_K)
    one_hot = (route_ids[:, :, None] == jnp.arange(expert_total, dtype=jnp.int32)).astype(jnp.int32)
    slot_rank = jnp.sum(one_hot * (jnp.cumsum(one_hot, axis=1) - 1), axis=-1)
    positions = route_ids * capacity + slot_rank
    owners = jnp.arange(quarter * TOP_K, dtype=jnp.int32) // TOP_K
    padded_rows = jnp.concatenate(
        [
            normed.reshape(head_ranks, quarter, model_width),
            jnp.zeros((head_ranks, 1, model_width), jnp.bfloat16),
        ],
        axis=1,
    ).reshape(head_ranks * (quarter + 1), model_width)
    slot_token = (
        jnp.full((head_ranks, routed_rows), quarter, jnp.int32)
        .at[jnp.arange(head_ranks, dtype=jnp.int32)[:, None], positions]
        .set(jnp.broadcast_to(owners[None, :], positions.shape))
    )
    slot_index = slot_token + (jnp.arange(head_ranks, dtype=jnp.int32) * (quarter + 1))[:, None]
    own_index = lax.dynamic_index_in_dim(slot_index, head_rank, 0, keepdims=True)
    outgoing = padded_rows[own_index].reshape(1, expert_ranks, slot_share, model_width)
    arrived = lax.all_to_all(outgoing, "ep", split_axis=1, concat_axis=1, tiled=True)
    piece_rows = lax.all_gather(
        arrived.reshape(1, expert_ranks, local_experts, capacity, model_width),
        "tp",
        axis=0,
        tiled=True,
    )
    gate_part = jnp.einsum(
        "tsecd,edf->tsecf", piece_rows, gate_weight, preferred_element_type=jnp.float32
    )
    up_part = jnp.einsum(
        "tsecd,edf->tsecf", piece_rows, up_weight, preferred_element_type=jnp.float32
    )
    hidden = (jax.nn.silu(gate_part) * up_part).astype(jnp.bfloat16)
    shared_hidden = (
        jax.nn.silu(jnp.dot(normed, shared_gate, preferred_element_type=jnp.float32))
        * jnp.dot(normed, shared_up, preferred_element_type=jnp.float32)
    ).astype(jnp.bfloat16)
    span_rows = routed_rows + quarter
    mixer_out = lax.psum_scatter(
        jnp.dot(heads_out, out_weight, preferred_element_type=jnp.float32).astype(jnp.bfloat16),
        "tp",
        scatter_dimension=0,
        tiled=True,
    )
    part_count = lax.axis_size("tp") * span_rows // span_rows
    routed_part = jnp.einsum(
        "tsecf,efd->tsecd", hidden, down_weight, preferred_element_type=jnp.float32
    ).reshape(part_count, routed_rows, model_width)
    shared_part = jnp.dot(shared_hidden, shared_down, preferred_element_type=jnp.float32).reshape(
        part_count, quarter, model_width
    )
    summed = lax.psum_scatter(
        jnp.concatenate([routed_part, shared_part], axis=1)
        .reshape(part_count * span_rows, model_width)
        .astype(jnp.bfloat16),
        "tp",
        scatter_dimension=0,
        tiled=True,
    )
    returned = lax.all_to_all(
        summed[:routed_rows].reshape(expert_ranks, slot_share, model_width),
        "ep",
        split_axis=0,
        concat_axis=0,
        tiled=True,
    ).reshape(routed_rows, model_width)
    own_positions = lax.dynamic_index_in_dim(positions, head_rank, 0, keepdims=False)
    picked = returned[own_positions].reshape(quarter, TOP_K, model_width).astype(jnp.float32)
    own_weights = lax.dynamic_slice_in_dim(route_weight, head_rank * quarter, quarter, 0)
    expert_out = (
        summed[routed_rows:].astype(jnp.float32) + jnp.sum(picked * own_weights[:, :, None], axis=1)
    ).astype(jnp.bfloat16)
    return (mixer_out, expert_out)


def shards(
    query_rows,
    key_rows,
    value_rows,
    query_gain,
    key_gain,
    sink_logit,
    out_weight,
    tokens,
    norm_gain,
    expert_ids,
    route_weight,
    gate_weight,
    up_weight,
    down_weight,
    shared_gate,
    shared_up,
    shared_down,
):
    expert_ranks = lax.axis_size("ep")
    head_ranks = lax.axis_size("tp")
    head_rank = lax.axis_index("tp")
    local_experts = gate_weight.shape[0]
    expert_total = local_experts * expert_ranks
    quarter = tokens.shape[0] // head_ranks
    model_width = tokens.shape[1]
    capacity = 2 * quarter * TOP_K // expert_total
    if head_ranks != 4 or capacity % 16 or expert_ranks % 2:
        return wide_shards(
            query_rows,
            key_rows,
            value_rows,
            query_gain,
            key_gain,
            sink_logit,
            out_weight,
            tokens,
            norm_gain,
            expert_ids,
            route_weight,
            gate_weight,
            up_weight,
            down_weight,
            shared_gate,
            shared_up,
            shared_down,
        )
    slot_share = local_experts * capacity
    routed_rows = expert_ranks * slot_share
    heads_out = attention_part(query_rows, key_rows, value_rows, query_gain, key_gain, sink_logit)
    mixer_part = jnp.dot(heads_out, out_weight, preferred_element_type=jnp.float32).astype(
        jnp.bfloat16
    )
    normed = rms_scale(tokens, norm_gain)
    shared_hidden = (
        jax.nn.silu(jnp.dot(normed, shared_gate, preferred_element_type=jnp.float32))
        * jnp.dot(normed, shared_up, preferred_element_type=jnp.float32)
    ).astype(jnp.bfloat16)
    shared_part = jnp.dot(shared_hidden, shared_down, preferred_element_type=jnp.float32).astype(
        jnp.bfloat16
    )
    own_ids = lax.dynamic_slice_in_dim(expert_ids, head_rank * quarter, quarter, 0)
    own_normed = lax.dynamic_slice_in_dim(normed, head_rank * quarter, quarter, 0)
    own_weights = lax.dynamic_slice_in_dim(route_weight, head_rank * quarter, quarter, 0)
    earlier = jnp.arange(quarter)[None, :] < jnp.arange(quarter)[:, None]
    columns = [own_ids[:, i] for i in range(TOP_K)]
    positions = []
    for ids in columns:
        rank_in = sum(
            jnp.sum(((ids[:, None] == other[None, :]) & earlier).astype(jnp.int32), axis=1)
            for other in columns
        )
        ahead = lax.rem(ids // local_experts - lax.axis_index("ep") + expert_ranks, expert_ranks)
        positions.append(ahead * slot_share + lax.rem(ids, local_experts) * capacity + rank_in)
    slots = jnp.arange(routed_rows, dtype=jnp.int32)
    chosen = sum((slots[:, None] == spot[None, :]).astype(jnp.bfloat16) for spot in positions)
    outgoing = jnp.dot(chosen, own_normed, preferred_element_type=jnp.float32).astype(jnp.bfloat16)
    returned, mixer_out, shared_out = exchange(
        outgoing.reshape(expert_ranks, slot_share, model_width),
        mixer_part.reshape(head_ranks, quarter, model_width),
        shared_part.reshape(head_ranks, quarter, model_width),
        gate_weight,
        up_weight,
        down_weight,
        capacity,
    )
    returned = returned.reshape(routed_rows, model_width)
    routed = sum(
        jnp.dot(
            (spot[:, None] == slots[None, :]).astype(jnp.bfloat16),
            returned,
            preferred_element_type=jnp.float32,
        )
        * own_weights[:, i : i + 1]
        for i, spot in enumerate(positions)
    )
    expert_out = (shared_out.astype(jnp.float32) + routed).astype(jnp.bfloat16)
    return (mixer_out, expert_out)


def solution(mesh):
    in_specs = (
        P("ep", "tp"),
        P("ep", "tp"),
        P("ep", "tp"),
        P(),
        P(),
        P("tp"),
        P("tp", None),
        P("ep", None),
        P(),
        P("ep", None),
        P("ep", None),
        P("ep", None, "tp"),
        P("ep", None, "tp"),
        P("ep", "tp", None),
        P(None, "tp"),
        P(None, "tp"),
        P("tp", None),
    )
    out_specs = (P(("ep", "tp"), None), P(("ep", "tp"), None))
    return jax.shard_map(shards, mesh=mesh, in_specs=in_specs, out_specs=out_specs, check_vma=False)
```

```python
import functools
import jax
import jax.numpy as jnp
from jax import lax
from jax.experimental import pallas as pl
from jax.experimental.pallas import tpu as pltpu
from jax.sharding import PartitionSpec as P

HEADS = 32
KV_HEADS = 8
HEAD_DIM = 64
WINDOW = 128
BLOCK = 128
TOP_K = 2


epsilon = 1e-06
masked_score = -1e30
score_scale = 0.125


def from_behind(block, axis, distance):
    devices = range(lax.axis_size(axis))
    route = [(i - distance, i) for i in devices if i - distance in devices]
    return lax.ppermute(block, axis, route)


def rms_scale(values, gain):
    widened = values.astype(jnp.float32)
    scaled = widened * lax.rsqrt(jnp.mean(widened * widened, axis=-1, keepdims=True) + epsilon)
    return (scaled * gain).astype(jnp.bfloat16)


def window_mask(first_block, block_count):
    query_pos = jnp.arange(BLOCK)[:, None]
    key_pos = jnp.arange(2 * BLOCK)[None, :]
    inside = (key_pos <= query_pos + BLOCK) & (key_pos > query_pos + BLOCK - WINDOW)
    not_first = (first_block + jnp.arange(block_count))[:, None, None] > 0
    return inside[None] & (not_first | (key_pos[None] >= BLOCK))


def band_blocks(rim_block, blocks_in):
    joined = jnp.concatenate([rim_block[None], blocks_in], axis=0)
    return jnp.concatenate([joined[:-1], joined[1:]], axis=1)


def attention_part(query_rows, key_rows, value_rows, query_gain, key_gain, sink_logit):
    sequence_rows = query_rows.shape[0]
    blocks = sequence_rows // BLOCK
    pair_heads = key_rows.shape[1] // HEAD_DIM
    group_size = HEADS // KV_HEADS
    query_normed = rms_scale(
        query_rows.reshape(blocks, BLOCK, pair_heads, group_size, HEAD_DIM), query_gain
    )
    key_normed = rms_scale(key_rows.reshape(blocks, BLOCK, pair_heads, HEAD_DIM), key_gain)
    value_blocks = value_rows.reshape(blocks, BLOCK, pair_heads, HEAD_DIM)
    rim_keys, rim_values = from_behind((key_normed[blocks - 1], value_blocks[blocks - 1]), "ep", 1)
    key_band = band_blocks(rim_keys, key_normed)
    value_band = band_blocks(rim_values, value_blocks)
    window = window_mask(lax.axis_index("ep") * blocks, blocks)
    scores = (
        jnp.einsum("nqhgd,nkhd->hgnqk", query_normed, key_band, preferred_element_type=jnp.float32)
        * score_scale
    )
    scores = jnp.where(window[None, None], scores, masked_score)
    sink_col = sink_logit.reshape(pair_heads, group_size, 1, 1, 1)
    row_max = jnp.maximum(jnp.max(scores, axis=-1, keepdims=True), sink_col)
    exp_scores = jnp.exp(scores - row_max)
    attn_probs = (
        exp_scores / (jnp.sum(exp_scores, axis=-1, keepdims=True) + jnp.exp(sink_col - row_max))
    ).astype(jnp.bfloat16)
    heads_out = (
        jnp.einsum("hgnqk,nkhd->nqhgd", attn_probs, value_band, preferred_element_type=jnp.float32)
        .astype(jnp.bfloat16)
        .reshape(sequence_rows, pair_heads * group_size * HEAD_DIM)
    )
    return heads_out


def exchange_kernel(
    ranks,
    group,
    local_experts,
    capacity,
    outgoing,
    outgoing_peer,
    mixer_part,
    shared_part,
    gate_hbm,
    up_hbm,
    down_hbm,
    returned,
    mixer_sum,
    shared_sum,
    rows,
    kept,
    sibling_send,
    sibling_recv,
    peer_send,
    peer_recv,
    finished,
    early_recv,
    early_send,
    early_peer,
    out_sems,
    in_sems,
    fan_send,
    fan_recv,
    add_send,
    add_recv,
    back_send,
    back_recv,
    early_s,
    early_r,
    own_sem,
    gate,
    up,
    down,
    weight_sem,
):
    rank = lax.axis_index("ep")
    part = lax.axis_index("tp")
    sibling = part + 1 - 2 * lax.rem(part, 2)
    peer = lax.rem(part + 2, 4)
    across = 3 - part
    f32, bf16 = jnp.float32, jnp.bfloat16
    mesh_ids = pl.DeviceIdType.MESH

    def partner(k, sign=1):
        half = ranks // 2
        return lax.rem(rank // 2 + half + sign * (k // 2), half) * 2 + lax.rem(
            lax.rem(rank, 2) + k, 2
        )

    def send(source, target, send_sem, recv_sem, ep_to, tp_to):
        copy = pltpu.make_async_remote_copy(
            src_ref=source,
            dst_ref=target,
            send_sem=send_sem,
            recv_sem=recv_sem,
            device_id=(ep_to, tp_to),
            device_id_type=mesh_ids,
        )
        copy.start()
        return copy

    barrier = pltpu.get_barrier_semaphore()
    for k in range(1, ranks):
        pl.semaphore_signal(
            barrier, inc=1, device_id=(partner(k), part), device_id_type=mesh_ids
        )
    for other in (sibling, peer):
        pl.semaphore_signal(barrier, inc=1, device_id=(rank, other), device_id_type=mesh_ids)
    pl.semaphore_wait(barrier, ranks + 1)

    own = pltpu.make_async_copy(outgoing.at[0], rows.at[0, 0], own_sem)
    own.start()
    to_sibling = {}
    to_peer = {}
    to_peer[1] = send(
        outgoing_peer.at[1], rows.at[1, 2], fan_send.at[0, 1], fan_recv.at[0, 1], partner(1), part
    )
    beside = pltpu.make_async_copy(outgoing_peer.at[0], rows.at[0, 2], fan_recv.at[0, 0])
    beside.start()
    dispatched = [None] + [
        send(
            outgoing.at[k],
            rows.at[k, 0],
            out_sems.at[k],
            in_sems.at[k],
            partner(k),
            part,
        )
        for k in range(1, ranks)
    ]
    early = []
    for i, full in enumerate((mixer_part, shared_part)):
        for j, which in enumerate((across, sibling)):
            s = 2 * i + j
            early.append(
                send(
                    full.at[which],
                    early_recv.at[s],
                    early_s.at[s],
                    early_r.at[s],
                    rank,
                    sibling,
                )
            )
    loads = [
        pltpu.make_async_copy(source, held, weight_sem.at[i])
        for i, (source, held) in enumerate(((gate_hbm, gate), (up_hbm, up), (down_hbm, down)))
    ]
    for load in loads:
        load.start()
    relayed = {}
    added = {}
    peered = {}
    backs = {}

    def fan_out(k):
        if k == 0:
            own.wait()
        else:
            dispatched[k].wait_recv()
        if k > 1:
            to_peer[k] = send(
                rows.at[k, 0], rows.at[k, 2], fan_send.at[0, k], fan_recv.at[0, k], rank, peer
            )
        to_sibling[k] = send(
            rows.at[k, 0], rows.at[k, 1], fan_send.at[1, k], fan_recv.at[1, k], rank, sibling
        )

    def relay(k):
        if k == 0:
            beside.wait()
        else:
            to_peer[k].wait_recv()
        relayed[k] = send(
            rows.at[k, 2], rows.at[k, 3], fan_send.at[2, k], fan_recv.at[2, k], rank, sibling
        )

    def early_add():
        for i, full in enumerate((mixer_part, shared_part)):
            early[2 * i].wait_recv()
            early_send[i] = (
                full[peer].astype(f32) + early_recv[2 * i].astype(f32)
            ).astype(bf16)
            early.append(
                send(
                    early_send.at[i],
                    early_peer.at[i],
                    early_s.at[4 + i],
                    early_r.at[4 + i],
                    rank,
                    peer,
                )
            )

    def early_finish():
        for i, (full, total) in enumerate(((mixer_part, mixer_sum), (shared_part, shared_sum))):
            early[2 * i + 1].wait_recv()
            early[4 + i].wait_recv()
            total[...] = (
                full[part].astype(f32)
                + early_recv[2 * i + 1].astype(f32)
                + early_peer[i].astype(f32)
            ).astype(bf16)

    def experts(g):
        first = g * group
        for k in range(first, first + group):
            to_sibling[k].wait_recv()
            relayed[k].wait_recv()
        if g == 0:
            for load in loads:
                load.wait()
        width = rows.shape[-1]

        def one(index, carry):
            at = pl.ds(pl.multiple_of(index * capacity, capacity), capacity)
            block = rows[first : first + group, :, at, :].reshape(group * 4 * capacity, width)
            gate_part = jnp.dot(block, gate[index], preferred_element_type=f32)
            up_part = jnp.dot(block, up[index], preferred_element_type=f32)
            hidden = (gate_part / (1.0 + jnp.exp(-gate_part)) * up_part).astype(bf16)
            made = jnp.dot(hidden, down[index], preferred_element_type=f32)
            made = made.astype(bf16).reshape(group, 4, capacity, width)
            spot = pl.ds(first, group)
            kept[spot, 0, at, :] = made[:, 0]
            sibling_send[spot, 0, at, :] = made[:, 1]
            kept[spot, 1, at, :] = made[:, 2]
            sibling_send[spot, 1, at, :] = made[:, 3]
            return carry

        lax.fori_loop(0, local_experts, one, 0)
        for k in range(first, first + group):
            added[k] = send(
                sibling_send.at[k],
                sibling_recv.at[k],
                add_send.at[0, k],
                add_recv.at[0, k],
                rank,
                sibling,
            )

    def pair_add(k):
        added[k].wait_recv()
        peer_send[k] = (kept[k, 1].astype(f32) + sibling_recv[k, 1].astype(f32)).astype(bf16)
        peered[k] = send(
            peer_send.at[k], peer_recv.at[k], add_send.at[1, k], add_recv.at[1, k], rank, peer
        )

    def finish(k):
        peered[k].wait_recv()
        total = (
            kept[k, 0].astype(f32) + sibling_recv[k, 0].astype(f32) + peer_recv[k].astype(f32)
        ).astype(bf16)
        if k == 0:
            returned[0] = total
        else:
            finished[k] = total
            backs[k] = send(
                finished.at[k],
                returned.at[k],
                back_send.at[k],
                back_recv.at[k],
                partner(k, -1),
                part,
            )

    groups = ranks // group
    for step in range(groups + 4):
        for stage, work in ((0, fan_out), (1, relay)):
            g = step - stage
            if 0 <= g < groups:
                for k in range(g * group, (g + 1) * group):
                    work(k)
        if step == 0:
            early_add()
        if 0 <= step - 3 < groups:
            for k in range((step - 3) * group, (step - 2) * group):
                pair_add(k)
        if 0 <= step - 2 < groups:
            experts(step - 2)
        if 0 <= step - 4 < groups:
            for k in range((step - 4) * group, (step - 3) * group):
                finish(k)
        if step == 2:
            early_finish()
    for k in range(1, ranks):
        backs[k].wait_recv()
    for k in range(1, ranks):
        dispatched[k].wait_send()
        backs[k].wait_send()
    for table in (to_peer, to_sibling, relayed, added, peered):
        for k in table:
            table[k].wait_send()
    for copy in early:
        copy.wait_send()


def exchange(outgoing, outgoing_peer, mixer_part, shared_part, gate, up, down, capacity):
    ranks, share, width = outgoing.shape
    quarter = mixer_part.shape[1]
    local_experts = gate.shape[0]
    group = 1
    bf16 = jnp.bfloat16
    dma = pltpu.SemaphoreType.DMA
    vmem = pl.BlockSpec(memory_space=pltpu.VMEM)
    return pl.pallas_call(
        functools.partial(exchange_kernel, ranks, group, local_experts, capacity),
        out_shape=(
            jax.ShapeDtypeStruct((ranks, share, width), bf16),
            jax.ShapeDtypeStruct((quarter, width), bf16),
            jax.ShapeDtypeStruct((quarter, width), bf16),
        ),
        in_specs=[vmem] * 4 + [pl.BlockSpec(memory_space=pl.ANY)] * 3,
        out_specs=(vmem,) * 3,
        scratch_shapes=[
            pltpu.VMEM((ranks, 4, share, width), bf16),
            pltpu.VMEM((ranks, 2, share, width), bf16),
            pltpu.VMEM((ranks, 2, share, width), bf16),
            pltpu.VMEM((ranks, 2, share, width), bf16),
            pltpu.VMEM((ranks, share, width), bf16),
            pltpu.VMEM((ranks, share, width), bf16),
            pltpu.VMEM((ranks, share, width), bf16),
            pltpu.VMEM((4, quarter, width), bf16),
            pltpu.VMEM((2, quarter, width), bf16),
            pltpu.VMEM((2, quarter, width), bf16),
            dma((ranks,)),
            dma((ranks,)),
            dma((3, ranks)),
            dma((3, ranks)),
            dma((2, ranks)),
            dma((2, ranks)),
            dma((ranks,)),
            dma((ranks,)),
            dma((6,)),
            dma((6,)),
            dma,
            pltpu.VMEM(gate.shape, bf16),
            pltpu.VMEM(up.shape, bf16),
            pltpu.VMEM(down.shape, bf16),
            dma((3,)),
        ],
        compiler_params=pltpu.CompilerParams(
            collective_id=0, has_side_effects=True, vmem_limit_bytes=64000 * 1024
        ),
    )(outgoing, outgoing_peer, mixer_part, shared_part, gate, up, down)


def wide_shards(
    query_rows,
    key_rows,
    value_rows,
    query_gain,
    key_gain,
    sink_logit,
    out_weight,
    tokens,
    norm_gain,
    expert_ids,
    route_weight,
    gate_weight,
    up_weight,
    down_weight,
    shared_gate,
    shared_up,
    shared_down,
):
    expert_ranks = lax.axis_size("ep")
    head_ranks = lax.axis_size("tp")
    head_rank = lax.axis_index("tp")
    sequence_rows = query_rows.shape[0]
    blocks = sequence_rows // BLOCK
    pair_heads = key_rows.shape[1] // HEAD_DIM
    group_size = HEADS // KV_HEADS
    query_normed = rms_scale(
        query_rows.reshape(blocks, BLOCK, pair_heads, group_size, HEAD_DIM), query_gain
    )
    key_normed = rms_scale(key_rows.reshape(blocks, BLOCK, pair_heads, HEAD_DIM), key_gain)
    value_blocks = value_rows.reshape(blocks, BLOCK, pair_heads, HEAD_DIM)
    rim_keys, rim_values = from_behind((key_normed[blocks - 1], value_blocks[blocks - 1]), "ep", 1)
    key_band = band_blocks(rim_keys, key_normed)
    value_band = band_blocks(rim_values, value_blocks)
    window = window_mask(lax.axis_index("ep") * blocks, blocks)
    scores = (
        jnp.einsum("nqhgd,nkhd->hgnqk", query_normed, key_band, preferred_element_type=jnp.float32)
        * score_scale
    )
    scores = jnp.where(window[None, None], scores, masked_score)
    sink_col = sink_logit.reshape(pair_heads, group_size, 1, 1, 1)
    row_max = jnp.maximum(jnp.max(scores, axis=-1, keepdims=True), sink_col)
    exp_scores = jnp.exp(scores - row_max)
    attn_probs = (
        exp_scores / (jnp.sum(exp_scores, axis=-1, keepdims=True) + jnp.exp(sink_col - row_max))
    ).astype(jnp.bfloat16)
    heads_out = (
        jnp.einsum("hgnqk,nkhd->nqhgd", attn_probs, value_band, preferred_element_type=jnp.float32)
        .astype(jnp.bfloat16)
        .reshape(sequence_rows, pair_heads * group_size * HEAD_DIM)
    )
    local_experts = gate_weight.shape[0]
    expert_total = local_experts * expert_ranks
    quarter = tokens.shape[0] // head_ranks
    model_width = tokens.shape[1]
    capacity = 2 * quarter * TOP_K // expert_total
    slot_share = local_experts * capacity
    routed_rows = expert_ranks * slot_share
    normed = rms_scale(tokens, norm_gain)
    route_ids = expert_ids.reshape(head_ranks, quarter * TOP_K)
    one_hot = (route_ids[:, :, None] == jnp.arange(expert_total, dtype=jnp.int32)).astype(jnp.int32)
    slot_rank = jnp.sum(one_hot * (jnp.cumsum(one_hot, axis=1) - 1), axis=-1)
    positions = route_ids * capacity + slot_rank
    owners = jnp.arange(quarter * TOP_K, dtype=jnp.int32) // TOP_K
    padded_rows = jnp.concatenate(
        [
            normed.reshape(head_ranks, quarter, model_width),
            jnp.zeros((head_ranks, 1, model_width), jnp.bfloat16),
        ],
        axis=1,
    ).reshape(head_ranks * (quarter + 1), model_width)
    slot_token = (
        jnp.full((head_ranks, routed_rows), quarter, jnp.int32)
        .at[jnp.arange(head_ranks, dtype=jnp.int32)[:, None], positions]
        .set(jnp.broadcast_to(owners[None, :], positions.shape))
    )
    slot_index = slot_token + (jnp.arange(head_ranks, dtype=jnp.int32) * (quarter + 1))[:, None]
    own_index = lax.dynamic_index_in_dim(slot_index, head_rank, 0, keepdims=True)
    outgoing = padded_rows[own_index].reshape(1, expert_ranks, slot_share, model_width)
    arrived = lax.all_to_all(outgoing, "ep", split_axis=1, concat_axis=1, tiled=True)
    piece_rows = lax.all_gather(
        arrived.reshape(1, expert_ranks, local_experts, capacity, model_width),
        "tp",
        axis=0,
        tiled=True,
    )
    gate_part = jnp.einsum(
        "tsecd,edf->tsecf", piece_rows, gate_weight, preferred_element_type=jnp.float32
    )
    up_part = jnp.einsum(
        "tsecd,edf->tsecf", piece_rows, up_weight, preferred_element_type=jnp.float32
    )
    hidden = (jax.nn.silu(gate_part) * up_part).astype(jnp.bfloat16)
    shared_hidden = (
        jax.nn.silu(jnp.dot(normed, shared_gate, preferred_element_type=jnp.float32))
        * jnp.dot(normed, shared_up, preferred_element_type=jnp.float32)
    ).astype(jnp.bfloat16)
    span_rows = routed_rows + quarter
    mixer_out = lax.psum_scatter(
        jnp.dot(heads_out, out_weight, preferred_element_type=jnp.float32).astype(jnp.bfloat16),
        "tp",
        scatter_dimension=0,
        tiled=True,
    )
    part_count = lax.axis_size("tp") * span_rows // span_rows
    routed_part = jnp.einsum(
        "tsecf,efd->tsecd", hidden, down_weight, preferred_element_type=jnp.float32
    ).reshape(part_count, routed_rows, model_width)
    shared_part = jnp.dot(shared_hidden, shared_down, preferred_element_type=jnp.float32).reshape(
        part_count, quarter, model_width
    )
    summed = lax.psum_scatter(
        jnp.concatenate([routed_part, shared_part], axis=1)
        .reshape(part_count * span_rows, model_width)
        .astype(jnp.bfloat16),
        "tp",
        scatter_dimension=0,
        tiled=True,
    )
    returned = lax.all_to_all(
        summed[:routed_rows].reshape(expert_ranks, slot_share, model_width),
        "ep",
        split_axis=0,
        concat_axis=0,
        tiled=True,
    ).reshape(routed_rows, model_width)
    own_positions = lax.dynamic_index_in_dim(positions, head_rank, 0, keepdims=False)
    picked = returned[own_positions].reshape(quarter, TOP_K, model_width).astype(jnp.float32)
    own_weights = lax.dynamic_slice_in_dim(route_weight, head_rank * quarter, quarter, 0)
    expert_out = (
        summed[routed_rows:].astype(jnp.float32) + jnp.sum(picked * own_weights[:, :, None], axis=1)
    ).astype(jnp.bfloat16)
    return (mixer_out, expert_out)


def shards(
    query_rows,
    key_rows,
    value_rows,
    query_gain,
    key_gain,
    sink_logit,
    out_weight,
    tokens,
    norm_gain,
    expert_ids,
    route_weight,
    gate_weight,
    up_weight,
    down_weight,
    shared_gate,
    shared_up,
    shared_down,
):
    expert_ranks = lax.axis_size("ep")
    head_ranks = lax.axis_size("tp")
    head_rank = lax.axis_index("tp")
    local_experts = gate_weight.shape[0]
    expert_total = local_experts * expert_ranks
    quarter = tokens.shape[0] // head_ranks
    model_width = tokens.shape[1]
    capacity = 2 * quarter * TOP_K // expert_total
    if head_ranks != 4 or capacity % 16 or expert_ranks % 2:
        return wide_shards(
            query_rows,
            key_rows,
            value_rows,
            query_gain,
            key_gain,
            sink_logit,
            out_weight,
            tokens,
            norm_gain,
            expert_ids,
            route_weight,
            gate_weight,
            up_weight,
            down_weight,
            shared_gate,
            shared_up,
            shared_down,
        )
    slot_share = local_experts * capacity
    routed_rows = expert_ranks * slot_share
    heads_out = attention_part(query_rows, key_rows, value_rows, query_gain, key_gain, sink_logit)
    mixer_part = jnp.dot(heads_out, out_weight, preferred_element_type=jnp.float32).astype(
        jnp.bfloat16
    )
    normed = rms_scale(tokens, norm_gain)
    shared_hidden = (
        jax.nn.silu(jnp.dot(normed, shared_gate, preferred_element_type=jnp.float32))
        * jnp.dot(normed, shared_up, preferred_element_type=jnp.float32)
    ).astype(jnp.bfloat16)
    shared_part = jnp.dot(shared_hidden, shared_down, preferred_element_type=jnp.float32).astype(
        jnp.bfloat16
    )
    rank = lax.axis_index("ep")
    earlier = jnp.arange(quarter)[None, :] < jnp.arange(quarter)[:, None]
    slots = jnp.arange(routed_rows, dtype=jnp.int32)

    def slot_rows(part, count):
        own_ids = lax.dynamic_slice_in_dim(expert_ids, part * quarter, quarter, 0)
        own_normed = lax.dynamic_slice_in_dim(normed, part * quarter, quarter, 0)
        columns = [own_ids[:, i] for i in range(TOP_K)]
        positions = []
        for ids in columns:
            rank_in = sum(
                jnp.sum(((ids[:, None] == other[None, :]) & earlier).astype(jnp.int32), axis=1)
                for other in columns
            )
            owner = ids // local_experts
            half = expert_ranks // 2
            ahead = 2 * lax.rem(owner // 2 - rank // 2 + half, half) + lax.rem(owner + rank, 2)
            positions.append(
                ahead * slot_share + lax.rem(ids, local_experts) * capacity + rank_in
            )
        used = slots[: count * slot_share]
        chosen = sum((used[:, None] == spot[None, :]).astype(jnp.bfloat16) for spot in positions)
        made = jnp.dot(chosen, own_normed, preferred_element_type=jnp.float32)
        return positions, made.astype(jnp.bfloat16).reshape(count, slot_share, model_width)

    positions, outgoing = slot_rows(head_rank, expert_ranks)
    _, outgoing_peer = slot_rows(lax.rem(head_rank + 2, 4), 2)
    own_weights = lax.dynamic_slice_in_dim(route_weight, head_rank * quarter, quarter, 0)
    returned, mixer_out, shared_out = exchange(
        outgoing,
        outgoing_peer,
        mixer_part.reshape(head_ranks, quarter, model_width),
        shared_part.reshape(head_ranks, quarter, model_width),
        gate_weight,
        up_weight,
        down_weight,
        capacity,
    )
    returned = returned.reshape(routed_rows, model_width)
    routed = sum(
        jnp.dot(
            (spot[:, None] == slots[None, :]).astype(jnp.bfloat16),
            returned,
            preferred_element_type=jnp.float32,
        )
        * own_weights[:, i : i + 1]
        for i, spot in enumerate(positions)
    )
    expert_out = (shared_out.astype(jnp.float32) + routed).astype(jnp.bfloat16)
    return (mixer_out, expert_out)


def solution(mesh):
    in_specs = (
        P("ep", "tp"),
        P("ep", "tp"),
        P("ep", "tp"),
        P(),
        P(),
        P("tp"),
        P("tp", None),
        P("ep", None),
        P(),
        P("ep", None),
        P("ep", None),
        P("ep", None, "tp"),
        P("ep", None, "tp"),
        P("ep", "tp", None),
        P(None, "tp"),
        P(None, "tp"),
        P("tp", None),
    )
    out_specs = (P(("ep", "tp"), None), P(("ep", "tp"), None))
    return jax.shard_map(shards, mesh=mesh, in_specs=in_specs, out_specs=out_specs, check_vma=False)
```
